32 devices in a mesh: sp: 8 (over z, y), tp: 4 (over x, core).
Axes of the slice: x: 2, y: 2, z: 4, core: 2. Of those that a mesh axis runs over, the one named last changes fastest.
Arguments:
- tokens: bfloat16 [8192, 4096], P('sp', 'tp'), may hold values from -16 to 16
- norm_gain: float32 [4096], replicated, may hold values from 0.1 to 1.9
- w_pool_in: bfloat16 [4096, 2048], P('sp', 'tp'), may hold values from -0.09375 to 0.09375
- w_query: bfloat16 [4096, 2048], P('sp', 'tp'), may hold values from -0.09375 to 0.09375
- w_key: bfloat16 [4096, 256], P('sp', 'tp'), may hold values from -0.09375 to 0.09375
- w_value: bfloat16 [4096, 256], P('sp', 'tp'), may hold values from -0.09375 to 0.09375
- pool_map: bfloat16 [4, 512, 512], P('tp'), may hold values from -0.25 to 0.25
- pool_scale: float32 [2048], P('tp'), may hold values from 0.3 to 3
- q_gain: float32 [64], replicated, may hold values from 0.1 to 1.9
- k_gain: float32 [64], replicated, may hold values from 0.1 to 1.9
- sinks: float32 [32], P('tp'), may hold values from 0 to 4
- w_out: bfloat16 [4096, 4096], P('tp', 'sp'), may hold values from -0.09375 to 0.09375
Outputs:
- layer_out: bfloat16 [8192, 4096], P(('sp', 'tp'))
The draws below stay inside these ranges and needn't reach their ends.
All inputs are finite; a program needn't handle non-finite values.
Results may differ from the reference program's by a relative error of at most 0.012.
Values may be sent and summed in bfloat16 or wider, within the bound.
A program may use at most 128 MiB of HBM per device.

```python
import math
import jax
import jax.numpy as jnp
from jax import lax

D = 4096
HEAD_DIM = 64
GROUP = 8
GROUPS = 4
WINDOW = 128
GROUP_WIDTH = 512
Q_HEADS = 32
BRANCH_WIDTH = 2048
MIX = 4096
TOKENS = 8192
N_TP = 4


def draw_tokens(key, part):
    first_key, second_key = jax.random.split(jax.random.fold_in(key, 11), 2)
    base_rows = jnp.clip(jax.random.normal(first_key, (TOKENS, D), jnp.float32), -5.0, 5.0)
    row_scale = jnp.exp(jax.random.uniform(second_key, (TOKENS, 1), jnp.float32, math.log(0.3), math.log(3.0)))
    return (base_rows * row_scale).astype(jnp.bfloat16)


def shard_levels(key, extent, pieces, least, high):
    def one(dim, shards_of):
        steps = jax.random.uniform(jax.random.fold_in(jax.random.fold_in(key, 6), dim), (shards_of,), jnp.float32, least / len(pieces), high / len(pieces))
        return jnp.repeat(jnp.exp(steps), extent[dim] // shards_of).reshape((-1,) + (1,) * (len(extent) - dim - 1))

    level = one(*pieces[0])
    for cut in pieces[1:]:
        level = level * one(*cut)
    return level


def gaussian(own_key, dims, scale, bound, cuts=(), held_as=jnp.bfloat16):
    drawn = jax.random.normal(own_key, dims, jnp.float32) * scale
    if len(cuts) > 0:
        drawn = shard_levels(own_key, dims, cuts, -0.22, 0.18) * drawn
    return jnp.clip(drawn, min=-bound, max=bound).astype(held_as)


def setup_inputs(seed: int = 0) -> dict:
    splits = jax.random.split(jax.random.key(seed), 13)
    return {
        "tokens": draw_tokens(jax.random.fold_in(splits[12], 71), 0),
        "norm_gain": jnp.clip(1.0 + 0.18 * jax.random.normal(splits[1], (D,), jnp.float32), 0.1, 1.9),
        "w_pool_in": gaussian(splits[2], (D, BRANCH_WIDTH), D ** -0.5, 0.09375, ((0, 8), (1, 4))),
        "w_query": gaussian(splits[3], (D, BRANCH_WIDTH), D ** -0.5, 0.09375, ((0, 8), (1, 4))),
        "w_key": gaussian(splits[4], (D, GROUPS * HEAD_DIM), D ** -0.5, 0.09375, ((0, 8), (1, 4))),
        "w_value": gaussian(splits[5], (D, GROUPS * HEAD_DIM), D ** -0.5, 0.09375, ((0, 8), (1, 4))),
        "pool_map": gaussian(splits[6], (GROUPS, GROUP_WIDTH, GROUP_WIDTH), GROUP_WIDTH ** -0.5, 0.25, ((0, 4),)),
        "pool_scale": jnp.clip(jnp.exp(math.log(3.0) - 2.3025851 * jax.random.uniform(splits[7], (BRANCH_WIDTH,), jnp.float32) ** shard_levels(splits[7], (BRANCH_WIDTH,), ((0, 4),), -0.2, 0.2)), 0.3, 3.0),
        "q_gain": jnp.clip(1.0 + 0.18 * jax.random.normal(splits[8], (HEAD_DIM,), jnp.float32), 0.1, 1.9),
        "k_gain": jnp.clip(1.0 + 0.18 * jax.random.normal(splits[9], (HEAD_DIM,), jnp.float32), 0.1, 1.9),
        "sinks": jnp.clip(4.0 * jax.random.uniform(splits[10], (Q_HEADS,), jnp.float32) ** shard_levels(splits[10], (Q_HEADS,), ((0, 4),), -0.2, 0.2), 0.0, 4.0),
        "w_out": gaussian(splits[11], (MIX, D), MIX ** -0.5, 0.09375, ((0, 4), (1, 8))),
    }


epsilon = 1e-06

def rms_scale(values):
    return values * lax.rsqrt(lax.optimization_barrier(jnp.mean(values * values, axis=-1, keepdims=True)) + epsilon)

def reference(tokens, norm_gain, w_pool_in, w_query, w_key, w_value, pool_map, pool_scale, q_gain, k_gain, sinks, w_out):
    widened = tokens.astype(jnp.float32)
    normed = (rms_scale(widened) * norm_gain).astype(jnp.bfloat16)
    pool_in = jnp.dot(normed, w_pool_in, preferred_element_type=jnp.float32).astype(jnp.bfloat16)
    query_rows = jnp.dot(normed, w_query, preferred_element_type=jnp.float32).astype(jnp.bfloat16)
    key_rows = jnp.dot(normed, w_key, preferred_element_type=jnp.float32).astype(jnp.bfloat16)
    value_rows = jnp.dot(normed, w_value, preferred_element_type=jnp.float32).astype(jnp.bfloat16)
    query_float = lax.optimization_barrier(query_rows).astype(jnp.float32).reshape(TOKENS, Q_HEADS, HEAD_DIM)
    query_normed = (rms_scale(query_float) * q_gain).astype(jnp.bfloat16)
    key_float = lax.optimization_barrier(key_rows).astype(jnp.float32).reshape(TOKENS, GROUPS, HEAD_DIM)
    key_normed = (rms_scale(key_float) * k_gain).astype(jnp.bfloat16)
    value_heads = value_rows.reshape(TOKENS, GROUPS, HEAD_DIM)
    positions = jnp.arange(TOKENS, dtype=jnp.int32)
    pool_float = pool_in.astype(jnp.float32).reshape(TOKENS, GROUPS, GROUP_WIDTH)
    padded = jnp.pad(pool_float, ((15, 0), (0, 0), (0, 0)))
    blocks = TOKENS // WINDOW
    key_padded = jnp.concatenate([jnp.zeros((WINDOW, GROUPS, HEAD_DIM), jnp.bfloat16), key_normed], axis=0)
    value_padded = jnp.concatenate([jnp.zeros((WINDOW, GROUPS, HEAD_DIM), jnp.bfloat16), value_heads], axis=0)
    query_pos = jnp.arange(WINDOW, dtype=jnp.int32)[:, None] + WINDOW
    key_pos = jnp.arange(2 * WINDOW, dtype=jnp.int32)[None, :]
    distance = query_pos - key_pos
    in_band = (distance >= 0) & (distance < WINDOW)
    key_global = jnp.arange(blocks, dtype=jnp.int32)[:, None] * WINDOW - WINDOW + jnp.arange(2 * WINDOW, dtype=jnp.int32)[None, :]
    allowed = in_band[None] & (key_global >= 0)[:, None, :]
    branches = []
    for group_index in range(GROUPS):
        span_width = 2 ** (group_index + 1)
        running = jnp.zeros((TOKENS, GROUP_WIDTH), jnp.float32)
        for offset in range(span_width):
            running = running + padded[15 - offset:15 - offset + TOKENS, group_index]
        counts = jnp.minimum(positions.astype(jnp.float32) + 1.0, float(span_width))
        pool_diff = (running / counts[:, None] - pool_float[:, group_index]).astype(jnp.bfloat16)
        mapped = jnp.dot(pool_diff, pool_map[group_index], preferred_element_type=jnp.float32)
        mapped = mapped * pool_scale[group_index * GROUP_WIDTH:(group_index + 1) * GROUP_WIDTH]
        pool_branch = rms_scale(mapped)
        head_first = group_index * GROUP
        query_blocks = query_normed[:, head_first:head_first + GROUP].reshape(blocks, WINDOW, GROUP, HEAD_DIM).astype(jnp.float32)
        key_pairs = jnp.concatenate([key_padded[:TOKENS, group_index].reshape(blocks, WINDOW, HEAD_DIM), key_padded[WINDOW:, group_index].reshape(blocks, WINDOW, HEAD_DIM)], axis=1).astype(jnp.float32)
        value_pairs = jnp.concatenate([value_padded[:TOKENS, group_index].reshape(blocks, WINDOW, HEAD_DIM), value_padded[WINDOW:, group_index].reshape(blocks, WINDOW, HEAD_DIM)], axis=1).astype(jnp.float32)
        scores = jnp.einsum('nqgd,nkd->ngqk', query_blocks, key_pairs) * HEAD_DIM ** (-0.5)
        head_ids = head_first + jnp.arange(GROUP, dtype=jnp.int32) + 1
        slopes = jnp.exp2(-8.0 * head_ids.astype(jnp.float32) / Q_HEADS)
        logits = scores - slopes[None, :, None, None] * distance.astype(jnp.float32)[None, None]
        exp_scores = jnp.exp(jnp.where(allowed[:, None], logits, -jnp.inf))
        sink_logits = sinks[head_first:head_first + GROUP]
        denominator = lax.optimization_barrier(jnp.sum(exp_scores, axis=-1)) + jnp.exp(sink_logits)[None, :, None]
        weights_bf = (exp_scores / denominator[..., None]).astype(jnp.bfloat16)
        attended = jnp.einsum('ngqk,nkd->nqgd', weights_bf.astype(jnp.float32), value_pairs)
        attn_branch = rms_scale(attended.reshape(TOKENS, GROUP_WIDTH))
        branches.append(jnp.stack([pool_branch, attn_branch], axis=1))
    mixed_rows = jnp.stack(branches, axis=1).reshape(TOKENS, MIX).astype(jnp.bfloat16)
    block_width = MIX // N_TP
    summed = jnp.zeros((TOKENS, D), jnp.float32)
    for part_index in range(N_TP):
        row_start = part_index * block_width
        partial_term = jnp.dot(mixed_rows[:, row_start:row_start + block_width], w_out[row_start:row_start + block_width], preferred_element_type=jnp.float32).astype(jnp.bfloat16)
        summed = summed + lax.optimization_barrier(partial_term).astype(jnp.float32)
    return summed.astype(jnp.bfloat16)
```

```python
import functools

import jax
import jax.numpy as jnp
from jax import lax
from jax.experimental import pallas as pl
from jax.experimental.pallas import tpu as pltpu
from jax.sharding import PartitionSpec as P

HEAD_DIM = 64
GROUP = 8
WINDOW = 128
GROUP_WIDTH = 512
Q_HEADS = 32


epsilon = 1e-06


def passed_along(value, axis, steps):
    count = lax.axis_size(axis)
    first, last = (max(0, -steps), min(count, count - steps))
    return lax.ppermute(value, axis, [(source, source + steps) for source in range(first, last)])


def rms_scale(values):
    return values * lax.rsqrt(jnp.mean(values * values, axis=-1, keepdims=True) + epsilon)


def ring_place(device, count):
    return jnp.where(device % 2 == 0, device // 2, count - 1 - device // 2)


def ring_device(place, count):
    place = (place + count) % count
    return jnp.where(place < count // 2, 2 * place, 2 * (count - 1 - place) + 1)


def partners():
    me = lax.axis_index("tp")
    return me, me + 1 - 2 * (me % 2), (me + 2) % 4


def greet(targets):
    barrier = pltpu.get_barrier_semaphore()
    for axis, target in targets:
        pl.semaphore_signal(
            barrier, inc=1, device_id={axis: target}, device_id_type=pl.DeviceIdType.MESH
        )
    pl.semaphore_wait(barrier, len(targets))


def remote(source, target, send_sem, recv_sem, axis, device):
    return pltpu.make_async_remote_copy(
        src_ref=source,
        dst_ref=target,
        send_sem=send_sem,
        recv_sem=recv_sem,
        device_id={axis: device},
        device_id_type=pl.DeviceIdType.MESH,
    )


TOKEN_CHUNKS = 4


def gather_kernel(
    count,
    tokens,
    weights,
    all_tokens,
    all_weights,
    own_sem,
    ring_send,
    ring_recv,
    near_send,
    near_recv,
    far_send,
    far_recv,
    pass_send,
    pass_recv,
):
    place = ring_place(lax.axis_index("sp"), count)
    right, left = ring_device(place + 1, count), ring_device(place - 1, count)
    me, partner, other = partners()
    rows, width = tokens.shape
    depth = weights.shape[0]
    half = depth // 2
    piece = rows // TOKEN_CHUNKS
    greet([("sp", right), ("sp", left), ("tp", partner), ("tp", other)])

    def token_at(chunk, owner):
        return all_tokens.at[
            pl.ds(chunk * piece, piece), pl.ds(pl.multiple_of(owner * width, width), width)
        ]

    def weight_at(owner, part):
        return all_weights.at[pl.ds(pl.multiple_of(owner * depth + part * half, half), half)]

    pending = []
    far = []
    for chunk in range(TOKEN_CHUNKS):
        copy = remote(
            tokens.at[pl.ds(chunk * piece, piece)],
            token_at(chunk, me),
            far_send.at[chunk],
            far_recv.at[chunk],
            "tp",
            other,
        )
        copy.start()
        far.append(copy)
    passed = []

    def pass_on(chunk):
        far[chunk].wait_recv()
        copy = remote(
            token_at(chunk, other),
            token_at(chunk, other),
            pass_send.at[chunk],
            pass_recv.at[chunk],
            "tp",
            partner,
        )
        copy.start()
        passed.append(copy)

    last = count // 2
    previous = {}
    for step in range(1, last + 1):
        current = {}
        for part in range(2):
            for way in range(2):
                if step == last and part != way:
                    continue
                sign = 1 - 2 * way
                if step == 1:
                    source = weights.at[pl.ds(part * half, half)]
                else:
                    previous[way, part].wait_recv()
                    source = weight_at(
                        ring_device(place - sign * (step - 1), count), part
                    )
                copy = remote(
                    source,
                    weight_at(ring_device(place - sign * (step - 1), count), part),
                    ring_send.at[way, step - 1, part],
                    ring_recv.at[way, step - 1, part],
                    "sp",
                    right if way == 0 else left,
                )
                copy.start()
                current[way, part] = copy
        pending += list(current.values())
        if step == last:
            for key, copy in previous.items():
                if key[0] != key[1]:
                    copy.wait_recv()
        previous = current
        if step == 1:
            near = remote(
                tokens,
                all_tokens.at[:, pl.ds(pl.multiple_of(me * width, width), width)],
                near_send,
                near_recv,
                "tp",
                partner,
            )
            near.start()
            own = [
                pltpu.make_async_copy(
                    tokens,
                    all_tokens.at[:, pl.ds(pl.multiple_of(me * width, width), width)],
                    own_sem.at[0],
                ),
                pltpu.make_async_copy(
                    weights,
                    all_weights.at[
                        pl.ds(pl.multiple_of(lax.axis_index("sp") * depth, depth), depth)
                    ],
                    own_sem.at[1],
                ),
            ]
            for copy in own:
                copy.start()
        if len(passed) < TOKEN_CHUNKS:
            pass_on(len(passed))
    while len(passed) < TOKEN_CHUNKS:
        pass_on(len(passed))
    for copy in previous.values():
        copy.wait_recv()
    for copy in pending + far:
        copy.wait_send()
    near.wait()
    for copy in passed:
        copy.wait()
    for copy in own:
        copy.wait()


def gather(tokens, weights):
    count = lax.axis_size("sp")
    rows, width = tokens.shape
    depth, columns = weights.shape
    dma = pltpu.SemaphoreType.DMA
    return pl.pallas_call(
        functools.partial(gather_kernel, count),
        out_shape=(
            jax.ShapeDtypeStruct((rows, width * lax.axis_size("tp")), tokens.dtype),
            jax.ShapeDtypeStruct((depth * count, columns), weights.dtype),
        ),
        in_specs=[pl.BlockSpec(memory_space=pltpu.VMEM)] * 2,
        out_specs=[pl.BlockSpec(memory_space=pl.ANY)] * 2,
        scratch_shapes=[
            dma((2,)),
            dma((2, count // 2, 2)),
            dma((2, count // 2, 2)),
            dma,
            dma,
            dma((TOKEN_CHUNKS,)),
            dma((TOKEN_CHUNKS,)),
            dma((TOKEN_CHUNKS,)),
            dma((TOKEN_CHUNKS,)),
        ],
        compiler_params=pltpu.CompilerParams(collective_id=0, has_side_effects=True),
        cost_estimate=pl.CostEstimate(
            flops=10**9, bytes_accessed=2 * count * depth * columns, transcendentals=0
        ),
    )(tokens, weights)


OUT_CHUNKS = 8


def project_kernel(
    mixed,
    w_out,
    out,
    send_near,
    recv_near,
    send_far,
    recv_far,
    own_terms,
    near_send,
    near_recv,
    far_send,
    far_recv,
):
    me, partner, other = partners()
    across = (partner + 2) % 4
    rows = out.shape[0]
    width = out.shape[1] // OUT_CHUNKS
    greet([("tp", partner), ("tp", other)])

    def term(block, chunk):
        return jnp.dot(
            mixed[pl.ds(pl.multiple_of(block * rows, rows), rows), :],
            w_out[:, pl.ds(pl.multiple_of(chunk * width, width), width)],
            preferred_element_type=jnp.float32,
        ).astype(jnp.bfloat16)

    def near_copy(chunk):
        return remote(
            send_near.at[chunk],
            recv_near.at[chunk],
            near_send.at[chunk],
            near_recv.at[chunk],
            "tp",
            partner,
        )

    def far_copy(chunk):
        return remote(
            send_far.at[chunk],
            recv_far.at[chunk],
            far_send.at[chunk],
            far_recv.at[chunk],
            "tp",
            other,
        )

    def first(chunk):
        send_near[chunk, 0] = term(across, chunk)
        send_near[chunk, 1] = term(partner, chunk)
        near_copy(chunk).start()
        own_terms[chunk, 0] = term(other, chunk)
        own_terms[chunk, 1] = term(me, chunk)

    def second(chunk):
        near_copy(chunk).wait_recv()
        send_far[chunk] = (
            own_terms[chunk, 0].astype(jnp.float32) + recv_near[chunk, 0].astype(jnp.float32)
        ).astype(jnp.bfloat16)
        far_copy(chunk).start()

    first(0)

    @pl.loop(1, OUT_CHUNKS)
    def _(chunk):
        first(chunk)
        second(chunk - 1)

    second(OUT_CHUNKS - 1)

    @pl.loop(0, OUT_CHUNKS)
    def _(chunk):
        far_copy(chunk).wait_recv()
        out[:, pl.ds(pl.multiple_of(chunk * width, width), width)] = (
            own_terms[chunk, 1].astype(jnp.float32)
            + recv_near[chunk, 1].astype(jnp.float32)
            + recv_far[chunk].astype(jnp.float32)
        ).astype(jnp.bfloat16)
        near_copy(chunk).wait_send()
        far_copy(chunk).wait_send()


def project(mixed, w_out):
    rows = mixed.shape[0] // 4
    width = w_out.shape[1] // OUT_CHUNKS
    dma = pltpu.SemaphoreType.DMA((OUT_CHUNKS,))
    return pl.pallas_call(
        project_kernel,
        out_shape=jax.ShapeDtypeStruct((rows, w_out.shape[1]), jnp.bfloat16),
        in_specs=[pl.BlockSpec(memory_space=pltpu.VMEM)] * 2,
        out_specs=pl.BlockSpec(memory_space=pltpu.VMEM),
        scratch_shapes=[
            pltpu.VMEM((OUT_CHUNKS, 2, rows, width), jnp.bfloat16),
            pltpu.VMEM((OUT_CHUNKS, 2, rows, width), jnp.bfloat16),
            pltpu.VMEM((OUT_CHUNKS, rows, width), jnp.bfloat16),
            pltpu.VMEM((OUT_CHUNKS, rows, width), jnp.bfloat16),
            pltpu.VMEM((OUT_CHUNKS, 2, rows, width), jnp.bfloat16),
            dma,
            dma,
            dma,
            dma,
        ],
        compiler_params=pltpu.CompilerParams(
            collective_id=1, has_side_effects=True, vmem_limit_bytes=60000 * 1024
        ),
        cost_estimate=pl.CostEstimate(
            flops=8 * mixed.shape[0] * w_out.shape[0] * w_out.shape[1] // 4,
            bytes_accessed=2 * w_out.size,
            transcendentals=0,
        ),
    )(mixed, w_out)


def local(
    tokens,
    norm_gain,
    w_pool_in,
    w_query,
    w_key,
    w_value,
    pool_map,
    pool_scale,
    q_gain,
    k_gain,
    sinks,
    w_out,
):
    tok_rows = tokens.shape[0]
    local_groups = w_key.shape[1] // HEAD_DIM
    seq_index = lax.axis_index("sp")
    group_first = lax.axis_index("tp") * local_groups
    out_columns = lax.all_gather(w_out, "sp", axis=1, tiled=True)
    weights = jnp.concatenate([w_pool_in, w_query, w_key, w_value], axis=1)
    gathered, all_weights = gather(tokens, weights)
    widened = gathered.astype(jnp.float32)
    normed = (rms_scale(widened) * norm_gain).astype(jnp.bfloat16)
    ext_rows = normed.shape[0]
    pool_end = w_pool_in.shape[1]
    query_end = pool_end + w_query.shape[1]
    key_end = query_end + w_key.shape[1]
    sums = jnp.dot(normed, all_weights, preferred_element_type=jnp.float32).astype(jnp.bfloat16)
    pool_sum, query_sum = sums[:, :pool_end], sums[:, pool_end:query_end]
    key_sum, value_sum = sums[:, query_end:key_end], sums[:, key_end:]
    pool_in = pool_sum.astype(jnp.bfloat16)
    query_rows = lax.optimization_barrier(query_sum.astype(jnp.bfloat16))
    key_rows = lax.optimization_barrier(key_sum.astype(jnp.bfloat16))
    value_rows = value_sum.astype(jnp.bfloat16).reshape(ext_rows, local_groups, HEAD_DIM)
    query_float = query_rows.astype(jnp.float32).reshape(ext_rows, local_groups * GROUP, HEAD_DIM)
    query_normed = (
        (rms_scale(query_float) * q_gain)
        .astype(jnp.bfloat16)
        .reshape(ext_rows, local_groups, GROUP, HEAD_DIM)
    )
    key_float = key_rows.astype(jnp.float32).reshape(ext_rows, local_groups, HEAD_DIM)
    key_normed = (rms_scale(key_float) * k_gain).astype(jnp.bfloat16)
    key_width = local_groups * HEAD_DIM
    pair_tail = jnp.concatenate(
        [
            key_normed[tok_rows - WINDOW :].reshape(WINDOW, key_width),
            value_rows[tok_rows - WINDOW :].reshape(WINDOW, key_width),
        ],
        axis=1,
    )
    earlier_pairs, earlier_pool = passed_along((pair_tail, pool_in[tok_rows - 15 :]), "sp", 1)
    key_span = jnp.concatenate(
        [earlier_pairs[:, :key_width].reshape(WINDOW, local_groups, HEAD_DIM), key_normed], axis=0
    )
    value_span = jnp.concatenate(
        [earlier_pairs[:, key_width:].reshape(WINDOW, local_groups, HEAD_DIM), value_rows], axis=0
    )
    pool_span = jnp.concatenate([earlier_pool, pool_in], axis=0)
    positions = seq_index * tok_rows + jnp.arange(tok_rows, dtype=jnp.int32)
    group_ids = group_first + jnp.arange(local_groups, dtype=jnp.int32)
    spans = jnp.exp2((group_ids + 1).astype(jnp.float32))
    pool_float = pool_span.astype(jnp.float32).reshape(tok_rows + 15, local_groups, GROUP_WIDTH)
    sum_two = pool_float[1:] + pool_float[:-1]
    sum_four = sum_two[2:] + sum_two[:-2]
    sum_eight = sum_four[4:] + sum_four[:-4]
    sum_sixteen = sum_eight[8:] + sum_eight[:-8]
    span_pick = spans[None, :, None]
    running = jnp.where(
        span_pick < 3.0,
        sum_two[14 : 14 + tok_rows],
        jnp.where(
            span_pick < 6.0,
            sum_four[12 : 12 + tok_rows],
            jnp.where(span_pick < 12.0, sum_eight[8 : 8 + tok_rows], sum_sixteen),
        ),
    )
    counts = jnp.minimum(positions.astype(jnp.float32)[:, None] + 1.0, spans[None, :])
    pool_diff = (running / counts[:, :, None] - pool_float[15:]).astype(jnp.bfloat16)
    mapped = jnp.einsum("tlc,lcd->tld", pool_diff, pool_map, preferred_element_type=jnp.float32)
    pool_branch = rms_scale(mapped * pool_scale.reshape(local_groups, GROUP_WIDTH))
    blocks = tok_rows // WINDOW
    query_blocks = query_normed.reshape(blocks, WINDOW, local_groups, GROUP, HEAD_DIM)
    key_pairs = jnp.concatenate(
        [
            key_span[:tok_rows].reshape(blocks, WINDOW, local_groups, HEAD_DIM),
            key_span[WINDOW:].reshape(blocks, WINDOW, local_groups, HEAD_DIM),
        ],
        axis=1,
    )
    value_pairs = jnp.concatenate(
        [
            value_span[:tok_rows].reshape(blocks, WINDOW, local_groups, HEAD_DIM),
            value_span[WINDOW:].reshape(blocks, WINDOW, local_groups, HEAD_DIM),
        ],
        axis=1,
    )
    scores = jnp.einsum(
        "nqlgd,nkld->nlgqk", query_blocks, key_pairs, preferred_element_type=jnp.float32
    ) * HEAD_DIM ** (-0.5)
    query_pos = jnp.arange(WINDOW, dtype=jnp.int32)[:, None] + WINDOW
    key_pos = jnp.arange(2 * WINDOW, dtype=jnp.int32)[None, :]
    distance = query_pos - key_pos
    in_band = (distance >= 0) & (distance < WINDOW)
    key_global = (
        seq_index * tok_rows
        + jnp.arange(blocks, dtype=jnp.int32)[:, None] * WINDOW
        - WINDOW
        + jnp.arange(2 * WINDOW, dtype=jnp.int32)[None, :]
    )
    allowed = in_band[None] & (key_global >= 0)[:, None, :]
    head_ids = group_ids[:, None] * GROUP + jnp.arange(GROUP, dtype=jnp.int32)[None, :] + 1
    slopes = jnp.exp2(-8.0 * head_ids.astype(jnp.float32) / Q_HEADS)
    logits = (
        scores - slopes[None, :, :, None, None] * distance.astype(jnp.float32)[None, None, None]
    )
    exp_scores = jnp.exp(jnp.where(allowed[:, None, None], logits, -jnp.inf))
    sink_logits = sinks.reshape(local_groups, GROUP)
    denominator = jnp.sum(exp_scores, axis=-1) + jnp.exp(sink_logits)[None, :, :, None]
    weights_bf = (exp_scores / denominator[..., None]).astype(jnp.bfloat16)
    attended = jnp.einsum(
        "nlgqk,nkld->nqlgd", weights_bf, value_pairs, preferred_element_type=jnp.float32
    )
    attn_branch = rms_scale(attended.reshape(tok_rows, local_groups, GROUP_WIDTH))
    mixed_rows = (
        jnp.stack([pool_branch, attn_branch], axis=2)
        .reshape(tok_rows, 2 * local_groups * GROUP_WIDTH)
        .astype(jnp.bfloat16)
    )
    return project(mixed_rows, out_columns)


def solution(mesh):
    in_specs = (
        P("sp", "tp"),
        P(),
        P("sp", "tp"),
        P("sp", "tp"),
        P("sp", "tp"),
        P("sp", "tp"),
        P("tp", None, None),
        P("tp"),
        P(),
        P(),
        P("tp"),
        P("tp", "sp"),
    )
    out_specs = P(("sp", "tp"), None)
    return jax.shard_map(local, mesh=mesh, in_specs=in_specs, out_specs=out_specs, check_vma=False)
```

```python
import functools

import jax
import jax.numpy as jnp
from jax import lax
from jax.experimental import pallas as pl
from jax.experimental.pallas import tpu as pltpu
from jax.sharding import PartitionSpec as P

HEAD_DIM = 64
GROUP = 8
WINDOW = 128
GROUP_WIDTH = 512
Q_HEADS = 32


epsilon = 1e-06


def passed_along(value, axis, steps):
    count = lax.axis_size(axis)
    first, last = (max(0, -steps), min(count, count - steps))
    return lax.ppermute(value, axis, [(source, source + steps) for source in range(first, last)])


def rms_scale(values):
    return values * lax.rsqrt(jnp.mean(values * values, axis=-1, keepdims=True) + epsilon)


def ring_place(device, count):
    return jnp.where(device % 2 == 0, device // 2, count - 1 - device // 2)


def ring_device(place, count):
    place = (place + count) % count
    return jnp.where(place < count // 2, 2 * place, 2 * (count - 1 - place) + 1)


def partners():
    me = lax.axis_index("tp")
    return me, me + 1 - 2 * (me % 2), (me + 2) % 4


def greet(targets):
    barrier = pltpu.get_barrier_semaphore()
    for axis, target in targets:
        pl.semaphore_signal(
            barrier, inc=1, device_id={axis: target}, device_id_type=pl.DeviceIdType.MESH
        )
    pl.semaphore_wait(barrier, len(targets))


def remote(source, target, send_sem, recv_sem, axis, device):
    return pltpu.make_async_remote_copy(
        src_ref=source,
        dst_ref=target,
        send_sem=send_sem,
        recv_sem=recv_sem,
        device_id={axis: device},
        device_id_type=pl.DeviceIdType.MESH,
    )


def ring_neighbours(count):
    place = ring_place(lax.axis_index("sp"), count)
    return ring_device(place + 1, count), ring_device(place - 1, count)


class Ring:
    def __init__(self, count, own_at, block_at, send, recv):
        self.count, self.last = count, count // 2
        self.place = ring_place(lax.axis_index("sp"), count)
        self.targets = ring_neighbours(count)
        self.own_at, self.block_at, self.send, self.recv = own_at, block_at, send, recv
        self.started, self.previous = [], {}

    def owner(self, distance):
        return ring_device(self.place - distance, self.count)

    def begin(self, step):
        current = {}
        for part in range(2):
            for way in range(2):
                if step == self.last and part != way:
                    continue
                owner = self.owner((1 - 2 * way) * (step - 1))
                if step > 1:
                    self.previous[way, part].wait_recv()
                copy = remote(
                    self.own_at(part) if step == 1 else self.block_at(owner, part),
                    self.block_at(owner, part),
                    self.send.at[way, step - 1, part],
                    self.recv.at[way, step - 1, part],
                    "sp",
                    self.targets[way],
                )
                copy.start()
                current[way, part] = copy
        if step == self.last:
            for key, copy in self.previous.items():
                if key[0] != key[1]:
                    copy.wait_recv()
        self.started += list(current.values())
        self.previous = current

    def arrive(self):
        for copy in self.previous.values():
            copy.wait_recv()

    def sent(self):
        for copy in self.started:
            copy.wait_send()

    def finish(self):
        self.arrive()
        self.sent()


TOKEN_CHUNKS = 4


def gather_kernel(
    count,
    tokens,
    weights,
    all_tokens,
    all_weights,
    own_sem,
    ring_send,
    ring_recv,
    near_send,
    near_recv,
    far_send,
    far_recv,
    pass_send,
    pass_recv,
):
    right, left = ring_neighbours(count)
    me, partner, other = partners()
    rows, width = tokens.shape
    depth = weights.shape[0]
    half = depth // 2
    piece = rows // TOKEN_CHUNKS
    greet([("sp", right), ("sp", left), ("tp", partner), ("tp", other)])

    def token_at(chunk, owner):
        return all_tokens.at[
            pl.ds(chunk * piece, piece), pl.ds(pl.multiple_of(owner * width, width), width)
        ]

    def weight_at(owner, part):
        return all_weights.at[pl.ds(pl.multiple_of(owner * depth + part * half, half), half)]

    far = []
    for chunk in range(TOKEN_CHUNKS):
        copy = remote(
            tokens.at[pl.ds(chunk * piece, piece)],
            token_at(chunk, me),
            far_send.at[chunk],
            far_recv.at[chunk],
            "tp",
            other,
        )
        copy.start()
        far.append(copy)
    passed = []

    def pass_on(chunk):
        far[chunk].wait_recv()
        copy = remote(
            token_at(chunk, other),
            token_at(chunk, other),
            pass_send.at[chunk],
            pass_recv.at[chunk],
            "tp",
            partner,
        )
        copy.start()
        passed.append(copy)

    ring = Ring(
        count,
        lambda part: weights.at[pl.ds(part * half, half)],
        weight_at,
        ring_send,
        ring_recv,
    )
    for step in range(1, ring.last + 1):
        ring.begin(step)
        if step == 1:
            near = remote(
                tokens,
                all_tokens.at[:, pl.ds(pl.multiple_of(me * width, width), width)],
                near_send,
                near_recv,
                "tp",
                partner,
            )
            near.start()
            own = [
                pltpu.make_async_copy(
                    tokens,
                    all_tokens.at[:, pl.ds(pl.multiple_of(me * width, width), width)],
                    own_sem.at[0],
                ),
                pltpu.make_async_copy(
                    weights,
                    all_weights.at[
                        pl.ds(pl.multiple_of(lax.axis_index("sp") * depth, depth), depth)
                    ],
                    own_sem.at[1],
                ),
            ]
            for copy in own:
                copy.start()
        if len(passed) < TOKEN_CHUNKS:
            pass_on(len(passed))
    while len(passed) < TOKEN_CHUNKS:
        pass_on(len(passed))
    ring.finish()
    for copy in far:
        copy.wait_send()
    near.wait()
    for copy in passed:
        copy.wait()
    for copy in own:
        copy.wait()


def gather(tokens, weights):
    count = lax.axis_size("sp")
    rows, width = tokens.shape
    depth, columns = weights.shape
    dma = pltpu.SemaphoreType.DMA
    return pl.pallas_call(
        functools.partial(gather_kernel, count),
        out_shape=(
            jax.ShapeDtypeStruct((rows, width * lax.axis_size("tp")), tokens.dtype),
            jax.ShapeDtypeStruct((depth * count, columns), weights.dtype),
        ),
        in_specs=[pl.BlockSpec(memory_space=pltpu.VMEM)] * 2,
        out_specs=[pl.BlockSpec(memory_space=pl.ANY)] * 2,
        scratch_shapes=[
            dma((2,)),
            dma((2, count // 2, 2)),
            dma((2, count // 2, 2)),
            dma,
            dma,
            dma((TOKEN_CHUNKS,)),
            dma((TOKEN_CHUNKS,)),
            dma((TOKEN_CHUNKS,)),
            dma((TOKEN_CHUNKS,)),
        ],
        compiler_params=pltpu.CompilerParams(collective_id=0, has_side_effects=True),
        cost_estimate=pl.CostEstimate(
            flops=10**9, bytes_accessed=2 * count * depth * columns, transcendentals=0
        ),
    )(tokens, weights)


def project_kernel(
    count,
    mixed,
    w_head,
    w_tail,
    out,
    tails,
    send_near,
    recv_near,
    send_far,
    recv_far,
    own_terms,
    ring_send,
    ring_recv,
    near_send,
    near_recv,
    far_send,
    far_recv,
):
    me, partner, other = partners()
    across = (partner + 2) % 4
    rows = out.shape[0]
    depth, width = w_tail.shape
    half = depth // 2
    head = w_head.shape[0]
    right, left = ring_neighbours(count)
    greet([("sp", right), ("sp", left), ("tp", partner), ("tp", other)])
    ring = Ring(
        count,
        lambda part: w_tail.at[pl.ds(part * half, half)],
        lambda owner, part: tails.at[owner, pl.ds(part * half, half)],
        ring_send,
        ring_recv,
    )
    ring.begin(1)

    def columns(owner):
        return pl.ds(pl.multiple_of(owner * width, width), width)

    def near_copy(chunk):
        return remote(
            send_near.at[chunk],
            recv_near.at[chunk],
            near_send.at[chunk],
            near_recv.at[chunk],
            "tp",
            partner,
        )

    def far_copy(chunk):
        return remote(
            send_far.at[chunk],
            recv_far.at[chunk],
            far_send.at[chunk],
            far_recv.at[chunk],
            "tp",
            other,
        )

    def first(chunk, owner, tail):
        def term(block):
            held = pl.ds(pl.multiple_of(block * rows, rows), rows)
            total = jnp.dot(
                mixed[held, :head], w_head[:, columns(owner)], preferred_element_type=jnp.float32
            )
            total += jnp.dot(mixed[held, head:], tail[...], preferred_element_type=jnp.float32)
            return total.astype(jnp.bfloat16)

        @pl.loop(0, 2)
        def _(pick):
            send_near[chunk, pick] = term(jnp.where(pick == 0, across, partner))

        near_copy(chunk).start()

        @pl.loop(0, 2)
        def _(pick):
            own_terms[chunk, pick] = term(jnp.where(pick == 0, other, me))

    def second(chunk):
        near_copy(chunk).wait_recv()
        send_far[chunk] = (
            own_terms[chunk, 0].astype(jnp.float32) + recv_near[chunk, 0].astype(jnp.float32)
        ).astype(jnp.bfloat16)
        far_copy(chunk).start()

    owners = [ring.owner(0)]
    first(0, owners[0], w_tail)
    second(0)
    for step in range(1, ring.last + 1):
        if step < ring.last:
            ring.begin(step + 1)
            fresh = [ring.owner(step), ring.owner(-step)]
        else:
            ring.arrive()
            fresh = [ring.owner(step)]
        start = len(owners)
        for extra, owner in enumerate(fresh):
            first(start + extra, owner, tails.at[owner])
        for extra in range(len(fresh)):
            second(start + extra)
        owners += fresh
    for chunk, owner in enumerate(owners):
        far_copy(chunk).wait_recv()
        out[:, columns(owner)] = (
            own_terms[chunk, 1].astype(jnp.float32)
            + recv_near[chunk, 1].astype(jnp.float32)
            + recv_far[chunk].astype(jnp.float32)
        ).astype(jnp.bfloat16)
    ring.sent()
    for chunk in range(count):
        near_copy(chunk).wait_send()
        far_copy(chunk).wait_send()


def project(mixed, w_head, w_tail):
    count = lax.axis_size("sp")
    rows = mixed.shape[0] // 4
    depth, width = w_tail.shape
    dma = pltpu.SemaphoreType.DMA
    return pl.pallas_call(
        functools.partial(project_kernel, count),
        out_shape=jax.ShapeDtypeStruct((rows, count * width), jnp.bfloat16),
        in_specs=[pl.BlockSpec(memory_space=pltpu.VMEM)] * 3,
        out_specs=pl.BlockSpec(memory_space=pltpu.VMEM),
        scratch_shapes=[
            pltpu.VMEM((count, depth, width), jnp.bfloat16),
            pltpu.VMEM((count, 2, rows, width), jnp.bfloat16),
            pltpu.VMEM((count, 2, rows, width), jnp.bfloat16),
            pltpu.VMEM((count, rows, width), jnp.bfloat16),
            pltpu.VMEM((count, rows, width), jnp.bfloat16),
            pltpu.VMEM((count, 2, rows, width), jnp.bfloat16),
            dma((2, count // 2, 2)),
            dma((2, count // 2, 2)),
            dma((count,)),
            dma((count,)),
            dma((count,)),
            dma((count,)),
        ],
        compiler_params=pltpu.CompilerParams(
            collective_id=1, has_side_effects=True, vmem_limit_bytes=60000 * 1024
        ),
        cost_estimate=pl.CostEstimate(
            flops=2 * mixed.size * count * width,
            bytes_accessed=2 * mixed.shape[1] * count * width,
            transcendentals=0,
        ),
    )(mixed, w_head, w_tail)


def local(
    tokens,
    norm_gain,
    w_pool_in,
    w_query,
    w_key,
    w_value,
    pool_map,
    pool_scale,
    q_gain,
    k_gain,
    sinks,
    w_out,
):
    tok_rows = tokens.shape[0]
    local_groups = w_key.shape[1] // HEAD_DIM
    seq_index = lax.axis_index("sp")
    group_first = lax.axis_index("tp") * local_groups
    weights = jnp.concatenate([w_pool_in, w_query, w_key, w_value], axis=1)
    gathered, all_weights = gather(tokens, weights)
    head = w_out.shape[0] // 2
    w_head, gathered = lax.optimization_barrier((w_out[:head], gathered))
    head_columns = lax.all_gather(w_head, "sp", axis=1, tiled=True)
    widened = gathered.astype(jnp.float32)
    normed = (rms_scale(widened) * norm_gain).astype(jnp.bfloat16)
    ext_rows = normed.shape[0]
    pool_end = w_pool_in.shape[1]
    query_end = pool_end + w_query.shape[1]
    key_end = query_end + w_key.shape[1]
    sums = jnp.dot(normed, all_weights, preferred_element_type=jnp.float32).astype(jnp.bfloat16)
    pool_sum, query_sum = sums[:, :pool_end], sums[:, pool_end:query_end]
    key_sum, value_sum = sums[:, query_end:key_end], sums[:, key_end:]
    pool_in = pool_sum.astype(jnp.bfloat16)
    query_rows = lax.optimization_barrier(query_sum.astype(jnp.bfloat16))
    key_rows = lax.optimization_barrier(key_sum.astype(jnp.bfloat16))
    value_rows = value_sum.astype(jnp.bfloat16).reshape(ext_rows, local_groups, HEAD_DIM)
    query_float = query_rows.astype(jnp.float32).reshape(ext_rows, local_groups * GROUP, HEAD_DIM)
    query_normed = (
        (rms_scale(query_float) * q_gain)
        .astype(jnp.bfloat16)
        .reshape(ext_rows, local_groups, GROUP, HEAD_DIM)
    )
    key_float = key_rows.astype(jnp.float32).reshape(ext_rows, local_groups, HEAD_DIM)
    key_normed = (rms_scale(key_float) * k_gain).astype(jnp.bfloat16)
    key_width = local_groups * HEAD_DIM
    pair_tail = jnp.concatenate(
        [
            key_normed[tok_rows - WINDOW :].reshape(WINDOW, key_width),
            value_rows[tok_rows - WINDOW :].reshape(WINDOW, key_width),
        ],
        axis=1,
    )
    earlier_pairs, earlier_pool = passed_along((pair_tail, pool_in[tok_rows - 15 :]), "sp", 1)
    key_span = jnp.concatenate(
        [earlier_pairs[:, :key_width].reshape(WINDOW, local_groups, HEAD_DIM), key_normed], axis=0
    )
    value_span = jnp.concatenate(
        [earlier_pairs[:, key_width:].reshape(WINDOW, local_groups, HEAD_DIM), value_rows], axis=0
    )
    pool_span = jnp.concatenate([earlier_pool, pool_in], axis=0)
    positions = seq_index * tok_rows + jnp.arange(tok_rows, dtype=jnp.int32)
    group_ids = group_first + jnp.arange(local_groups, dtype=jnp.int32)
    spans = jnp.exp2((group_ids + 1).astype(jnp.float32))
    pool_float = pool_span.astype(jnp.float32).reshape(tok_rows + 15, local_groups, GROUP_WIDTH)
    sum_two = pool_float[1:] + pool_float[:-1]
    sum_four = sum_two[2:] + sum_two[:-2]
    sum_eight = sum_four[4:] + sum_four[:-4]
    sum_sixteen = sum_eight[8:] + sum_eight[:-8]
    span_pick = spans[None, :, None]
    running = jnp.where(
        span_pick < 3.0,
        sum_two[14 : 14 + tok_rows],
        jnp.where(
            span_pick < 6.0,
            sum_four[12 : 12 + tok_rows],
            jnp.where(span_pick < 12.0, sum_eight[8 : 8 + tok_rows], sum_sixteen),
        ),
    )
    counts = jnp.minimum(positions.astype(jnp.float32)[:, None] + 1.0, spans[None, :])
    pool_diff = (running / counts[:, :, None] - pool_float[15:]).astype(jnp.bfloat16)
    mapped = jnp.einsum("tlc,lcd->tld", pool_diff, pool_map, preferred_element_type=jnp.float32)
    pool_branch = rms_scale(mapped * pool_scale.reshape(local_groups, GROUP_WIDTH))
    blocks = tok_rows // WINDOW
    query_blocks = query_normed.reshape(blocks, WINDOW, local_groups, GROUP, HEAD_DIM)
    key_pairs = jnp.concatenate(
        [
            key_span[:tok_rows].reshape(blocks, WINDOW, local_groups, HEAD_DIM),
            key_span[WINDOW:].reshape(blocks, WINDOW, local_groups, HEAD_DIM),
        ],
        axis=1,
    )
    value_pairs = jnp.concatenate(
        [
            value_span[:tok_rows].reshape(blocks, WINDOW, local_groups, HEAD_DIM),
            value_span[WINDOW:].reshape(blocks, WINDOW, local_groups, HEAD_DIM),
        ],
        axis=1,
    )
    scores = jnp.einsum(
        "nqlgd,nkld->nlgqk", query_blocks, key_pairs, preferred_element_type=jnp.float32
    ) * HEAD_DIM ** (-0.5)
    query_pos = jnp.arange(WINDOW, dtype=jnp.int32)[:, None] + WINDOW
    key_pos = jnp.arange(2 * WINDOW, dtype=jnp.int32)[None, :]
    distance = query_pos - key_pos
    in_band = (distance >= 0) & (distance < WINDOW)
    key_global = (
        seq_index * tok_rows
        + jnp.arange(blocks, dtype=jnp.int32)[:, None] * WINDOW
        - WINDOW
        + jnp.arange(2 * WINDOW, dtype=jnp.int32)[None, :]
    )
    allowed = in_band[None] & (key_global >= 0)[:, None, :]
    head_ids = group_ids[:, None] * GROUP + jnp.arange(GROUP, dtype=jnp.int32)[None, :] + 1
    slopes = jnp.exp2(-8.0 * head_ids.astype(jnp.float32) / Q_HEADS)
    logits = (
        scores - slopes[None, :, :, None, None] * distance.astype(jnp.float32)[None, None, None]
    )
    exp_scores = jnp.exp(jnp.where(allowed[:, None, None], logits, -jnp.inf))
    sink_logits = sinks.reshape(local_groups, GROUP)
    denominator = jnp.sum(exp_scores, axis=-1) + jnp.exp(sink_logits)[None, :, :, None]
    weights_bf = (exp_scores / denominator[..., None]).astype(jnp.bfloat16)
    attended = jnp.einsum(
        "nlgqk,nkld->nqlgd", weights_bf, value_pairs, preferred_element_type=jnp.float32
    )
    attn_branch = rms_scale(attended.reshape(tok_rows, local_groups, GROUP_WIDTH))
    mixed_rows = (
        jnp.stack([pool_branch, attn_branch], axis=2)
        .reshape(tok_rows, 2 * local_groups * GROUP_WIDTH)
        .astype(jnp.bfloat16)
    )
    return project(mixed_rows, head_columns, w_out[head:])


def solution(mesh):
    in_specs = (
        P("sp", "tp"),
        P(),
        P("sp", "tp"),
        P("sp", "tp"),
        P("sp", "tp"),
        P("sp", "tp"),
        P("tp", None, None),
        P("tp"),
        P(),
        P(),
        P("tp"),
        P("tp", "sp"),
    )
    out_specs = P(("sp", "tp"), None)
    return jax.shard_map(local, mesh=mesh, in_specs=in_specs, out_specs=out_specs, check_vma=False)
```
